32 devices in a mesh: sp: 4 (over z), fs: 4 (over y, x), tp: 2 (over core).
Axes of the slice: x: 2, y: 2, z: 4, core: 2. Of those that a mesh axis runs over, the one named last changes fastest.
Arguments:
- tokens: bfloat16 [4096, 2048], P(('fs', 'sp')), parts along dimension 0, may hold values from -6 to 6
- norm_gain: float32 [2048], replicated, may hold values from 0.1 to 1.9
- w_query: bfloat16 [2048, 1024], P('sp', 'tp'), may hold values from -0.080939698 to 0.080939698
- w_key: bfloat16 [2048, 256], P('sp', 'tp'), may hold values from -0.080939698 to 0.080939698
- w_value: bfloat16 [2048, 256], P('sp', 'tp'), may hold values from -0.125 to 0.125
- w_conv_in: bfloat16 [2048, 1024], P('sp', 'tp'), may hold values from -0.125 to 0.125
- w_conv_gate: bfloat16 [2048, 1024], P('sp', 'tp'), may hold values from -0.125 to 0.125
- sink_logit: float32 [16], P('tp'), may hold values from 2 to 6
- conv_taps: float32 [31, 1024], P(None, 'tp'), may hold values from -5.3881591 to 5.3881591
- conv_bias: float32 [1024], P('tp'), may hold values from -0.9 to 5.9
- channel_gain: float32 [1024], P('tp'), may hold values from 0.1 to 1.9
- channel_shift: float32 [1024], P('tp'), may hold values from -3 to 3
- w_attn_out: bfloat16 [1024, 2048], P(None, 'sp'), may hold values from -1.5 to 1.5
- w_conv_out: bfloat16 [1024, 2048], P(None, 'sp'), may hold values from -0.1875 to 0.1875
Outputs:
- output: bfloat16 [4096, 2048], P(('fs', 'sp', 'tp')), parts along dimension 0
The draws below stay inside these ranges and needn't reach their ends.
There are 4 independent parts, one for each index of `fs`. The reference program is written for one: setup_inputs(seed, part) draws one part's arguments, and reference() takes and returns one part's arrays. A program takes and returns all parts, laid end to end along the dimension named above; an argument that names none is the same for every part. Nothing has to cross between parts.
All inputs are finite; a program needn't handle non-finite values.
Results may differ from the reference program's by a relative error of at most 0.011.
Values may be sent and summed in bfloat16 or wider, within the bound.
A program may use at most 64 MiB of HBM per device.

```python
import jax
import jax.numpy as jnp
from jax import lax

D = 2048
HEADS = 16
KV_HEADS = 4
HEAD_DIM = 64
CHANNELS = 1024
TAPS = 31
WINDOW = 128
GRID_W = 64
TOK_DEV = 256
SEQ = 1024
ATT_WIDTH = 1024
KV_WIDTH = 256


def draw_tokens(key, part):
    noise_key = jax.random.fold_in(key, 0)
    result = jnp.clip(jax.random.normal(noise_key, (SEQ, D), jnp.float32), -6.0, 6.0)
    return result.astype(jnp.bfloat16)


def draw_w_query(key, part):
    base = jnp.clip(jax.random.normal(jax.random.fold_in(key, 11), (D, HEADS * HEAD_DIM), jnp.float32), -3.0, 3.0) * D ** (-0.5)
    return base.astype(jnp.bfloat16)


def draw_w_key(key, part):
    base = jnp.clip(jax.random.normal(jax.random.fold_in(key, 12), (D, KV_HEADS * HEAD_DIM), jnp.float32), -3.0, 3.0) * D ** (-0.5)
    return base.astype(jnp.bfloat16)


def draw_conv_taps(key, part):
    base_key, jitter_key = jax.random.split(jax.random.fold_in(key, 13))
    base = jnp.clip(jax.random.normal(base_key, (TAPS, CHANNELS), jnp.float32), -3.0, 3.0)
    order = jnp.arange(CHANNELS, dtype=jnp.float32) / CHANNELS
    jitter = jnp.clip(jax.random.normal(jitter_key, (CHANNELS,), jnp.float32), -3.0, 3.0)
    exponent = jnp.clip(order + 0.15 * jitter, 0.0, 1.0)
    return (base * TAPS ** (-0.5) * 10.0 ** exponent[None, :]).astype(jnp.float32)


def draw_conv_bias(key, part):
    order = jnp.arange(CHANNELS, dtype=jnp.float32) / CHANNELS
    jitter = jnp.clip(jax.random.normal(jax.random.fold_in(key, 14), (CHANNELS,), jnp.float32), -3.0, 3.0)
    ramp = 3.0 * order
    return (ramp + 0.3 * jitter).astype(jnp.float32)


def levels(rng, shape, pieces, smallest, largest):
    factor_of = 1.0
    for axis_at, shards_of in pieces:
        draws = jax.random.uniform(jax.random.fold_in(jax.random.fold_in(rng, 6), axis_at), (shards_of,), jnp.float32, smallest / len(pieces), largest / len(pieces))
        factor_of = factor_of * jnp.repeat(jnp.exp(draws), shape[axis_at] // shards_of).reshape((-1,) + (1,) * (len(shape) - 1 - axis_at))
    return factor_of


def normal_values(key, shape, deviation, limit, cuts=(), held_as=jnp.bfloat16):
    array = deviation * jax.random.normal(key, shape, jnp.float32)
    if cuts:
        array = array * levels(key, shape, cuts, -0.22, 0.18)
    return jnp.clip(array, -limit, limit).astype(held_as)


def setup_inputs(seed: int = 0, part: int = 0) -> dict:
    arg_keys = jax.random.split(jax.random.key(seed), 15)
    part_keys = jax.random.split(jax.random.fold_in(arg_keys[14], part), 15)
    tokens = draw_tokens(jax.random.fold_in(jax.random.fold_in(arg_keys[14], part), 71), part)
    norm_gain = jnp.clip(1.0 + 0.18 * jax.random.normal(arg_keys[1], (D,), jnp.float32), 0.1, 1.9)
    w_query = draw_w_query(jax.random.fold_in(arg_keys[14], 71), part)
    w_key = draw_w_key(jax.random.fold_in(arg_keys[14], 71), part)
    w_value = normal_values(arg_keys[4], (D, KV_WIDTH), D ** -0.5, 0.125, ((0, 4), (1, 2)))
    w_conv_in = normal_values(arg_keys[5], (D, CHANNELS), D ** -0.5, 0.125, ((0, 4), (1, 2)))
    w_conv_gate = normal_values(arg_keys[6], (D, CHANNELS), D ** -0.5, 0.125, ((0, 4), (1, 2)))
    sink_logit = jnp.clip(2.0 + 4.0 * jax.random.uniform(arg_keys[7], (HEADS,), jnp.float32) ** levels(arg_keys[7], (HEADS,), ((0, 2),), -0.2, 0.2), 2.0, 6.0)
    conv_taps = draw_conv_taps(jax.random.fold_in(arg_keys[14], 71), part)
    conv_bias = draw_conv_bias(jax.random.fold_in(arg_keys[14], 71), part)
    channel_gain = jnp.clip(1.0 + 0.18 * jax.random.normal(arg_keys[10], (CHANNELS,), jnp.float32), 0.1, 1.9)
    channel_shift = normal_values(arg_keys[11], (CHANNELS,), 0.5, 3.0, ((0, 2),), jnp.float32)
    w_attn_out = normal_values(arg_keys[12], (ATT_WIDTH, D), (max(ATT_WIDTH // 64, 1)) ** -0.5, 1.5, ((1, 4),))
    w_conv_out = normal_values(arg_keys[13], (CHANNELS, D), CHANNELS ** -0.5, 0.1875, ((1, 4),))
    return {"tokens": tokens, "norm_gain": norm_gain, "w_query": w_query, "w_key": w_key, "w_value": w_value, "w_conv_in": w_conv_in, "w_conv_gate": w_conv_gate, "sink_logit": sink_logit, "conv_taps": conv_taps, "conv_bias": conv_bias, "channel_gain": channel_gain, "channel_shift": channel_shift, "w_attn_out": w_attn_out, "w_conv_out": w_conv_out}


EPSILON = 1e-06
NEGATIVE = -1e+30
ROPE_BASE = 10000.0

def rotate_pairs(values, positions):
    middle = values.shape[-1] // 2
    inverse = ROPE_BASE ** (-jnp.arange(middle, dtype=jnp.float32) / middle)
    angles = positions.astype(jnp.float32)[:, None] * inverse[None, :]
    cosine = jnp.cos(angles)[:, None, :]
    sine_table = jnp.sin(angles)[:, None, :]
    leading = values[..., :middle]
    trailing = values[..., middle:]
    return jnp.concatenate([leading * cosine - trailing * sine_table, leading * sine_table + trailing * cosine], axis=-1)

def grid_rotate(values, positions):
    middle = values.shape[-1] // 2
    return jnp.concatenate([rotate_pairs(values[..., :middle], positions // GRID_W), rotate_pairs(values[..., middle:], positions % GRID_W)], axis=-1)

def reference(tokens, norm_gain, w_query, w_key, w_value, w_conv_in, w_conv_gate, sink_logit, conv_taps, conv_bias, channel_gain, channel_shift, w_attn_out, w_conv_out):
    total = tokens.shape[0]
    token_float = tokens.astype(jnp.float32)
    normed = (token_float * lax.rsqrt(lax.optimization_barrier(jnp.mean(token_float * token_float, axis=-1, keepdims=True)) + EPSILON) * norm_gain[None, :]).astype(jnp.bfloat16)
    positions = jnp.arange(total, dtype=jnp.int32)
    group = HEADS // KV_HEADS
    query = jnp.dot(normed, w_query, preferred_element_type=jnp.float32).reshape(total, HEADS, HEAD_DIM)
    query = grid_rotate(query, positions).astype(jnp.bfloat16)
    keys = jnp.dot(normed, w_key, preferred_element_type=jnp.float32).reshape(total, KV_HEADS, HEAD_DIM)
    keys = grid_rotate(keys, positions).astype(jnp.bfloat16)
    values = jnp.dot(normed, w_value, preferred_element_type=jnp.float32).astype(jnp.bfloat16)
    values = values.reshape(total, KV_HEADS, HEAD_DIM)
    padded_keys = jnp.pad(keys, ((WINDOW, WINDOW), (0, 0), (0, 0)))
    padded_values = jnp.pad(values, ((WINDOW, WINDOW), (0, 0), (0, 0)))
    block = min(TOK_DEV, 512)
    span = block + 2 * WINDOW
    sinks = sink_logit.astype(jnp.float32).reshape(KV_HEADS, group)[:, :, None, None]

    def attend(block_index):
        start = (block_index * block).astype(jnp.int32)
        queries = lax.dynamic_slice_in_dim(query, start, block, 0).reshape(block, KV_HEADS, group, HEAD_DIM)
        near_keys = lax.dynamic_slice_in_dim(padded_keys, start, span, 0)
        near_values = lax.dynamic_slice_in_dim(padded_values, start, span, 0)
        scores = jnp.einsum('qkgd,skd->kgqs', queries.astype(jnp.float32), near_keys.astype(jnp.float32)) * HEAD_DIM ** (-0.5)
        query_pos = start + jnp.arange(block, dtype=jnp.int32)
        key_pos = start - WINDOW + jnp.arange(span, dtype=jnp.int32)
        valid = (jnp.abs(query_pos[:, None] - key_pos[None, :]) <= WINDOW) & (key_pos[None, :] >= 0) & (key_pos[None, :] < total)
        scores = jnp.where(valid[None, None], scores, NEGATIVE)
        top = jnp.maximum(lax.optimization_barrier(jnp.max(scores, axis=-1, keepdims=True)), sinks)
        raised = jnp.exp(scores - top)
        denominator = lax.optimization_barrier(jnp.sum(raised, axis=-1, keepdims=True)) + jnp.exp(sinks - top)
        probs = (raised / denominator).astype(jnp.bfloat16)
        mixed = jnp.einsum('kgqs,skd->qkgd', probs.astype(jnp.float32), near_values.astype(jnp.float32))
        return mixed.astype(jnp.bfloat16).reshape(block, HEADS * HEAD_DIM)
    attended = lax.map(attend, jnp.arange(total // block, dtype=jnp.int32)).reshape(total, HEADS * HEAD_DIM)
    glu = (jnp.dot(normed, w_conv_in, preferred_element_type=jnp.float32) * jax.nn.sigmoid(jnp.dot(normed, w_conv_gate, preferred_element_type=jnp.float32))).astype(jnp.bfloat16)
    reach = TAPS // 2
    padded_glu = jnp.pad(glu.astype(jnp.float32), ((reach, reach), (0, 0)))
    filtered = jnp.zeros((total, CHANNELS), jnp.float32) + conv_bias[None, :]
    for offset in range(TAPS):
        filtered = filtered + conv_taps[offset][None, :] * padded_glu[offset:offset + total]
    centre = lax.optimization_barrier(jnp.mean(filtered, axis=-1, keepdims=True))
    centred = filtered - centre
    spread = lax.optimization_barrier(jnp.mean(centred * centred, axis=-1, keepdims=True))
    conv_out = jax.nn.silu(centred * lax.rsqrt(spread + EPSILON) * channel_gain[None, :] + channel_shift[None, :]).astype(jnp.bfloat16)
    result = jnp.dot(attended, w_attn_out, preferred_element_type=jnp.float32) + jnp.dot(conv_out, w_conv_out, preferred_element_type=jnp.float32)
    return result.astype(jnp.bfloat16)
```

```python
import jax
import jax.numpy as jnp
from jax import lax
from jax.sharding import PartitionSpec as P

HEAD_DIM = 64
WINDOW = 128
GRID_W = 64


EPSILON = 1e-06
NEGATIVE = -1e30
ROPE_BASE = 10000.0


def padded(block, sides, width):
    for axis, dim in sides:
        count = lax.axis_size(axis)
        forward = [(i, i + 1) for i in range(count - 1)]
        backward = [(target, source) for source, target in forward]
        low = lax.ppermute(
            lax.slice_in_dim(block, block.shape[dim] - width, None, axis=dim), axis, forward
        )
        high = lax.ppermute(lax.slice_in_dim(block, 0, width, axis=dim), axis, backward)
        block = jnp.concatenate([low, block, high], axis=dim)
    return block


def rotate_pairs(values, positions):
    middle = values.shape[-1] // 2
    inverse = ROPE_BASE ** (-jnp.arange(middle, dtype=jnp.float32) / middle)
    angles = positions.astype(jnp.float32)[:, None] * inverse[None, :]
    cosine = jnp.cos(angles)[:, None, :]
    sine_table = jnp.sin(angles)[:, None, :]
    leading = values[..., :middle]
    trailing = values[..., middle:]
    return jnp.concatenate(
        [leading * cosine - trailing * sine_table, leading * sine_table + trailing * cosine],
        axis=-1,
    )


def grid_rotate(values, positions):
    middle = values.shape[-1] // 2
    return jnp.concatenate(
        [
            rotate_pairs(values[..., :middle], positions // GRID_W),
            rotate_pairs(values[..., middle:], positions % GRID_W),
        ],
        axis=-1,
    )


def gather_inputs(normed, packed_in):
    return (
        lax.all_gather(normed, ("fs", "tp"), axis=0, tiled=True),
        lax.all_gather(packed_in, "sp", axis=0, tiled=True),
    )


def gather_outputs(packed_out, after):
    return lax.all_gather(packed_out, "sp", axis=1, tiled=True)


def gather_stats(pair):
    return lax.all_gather(pair, ("fs", "tp"), axis=0)


def scatter_sum(features, whole_out):
    partial = jnp.dot(features, whole_out, preferred_element_type=jnp.float32)
    return lax.psum_scatter(
        partial.astype(jnp.bfloat16), ("fs", "tp"), scatter_dimension=0, tiled=True
    )


def local(
    tokens,
    norm_gain,
    w_query,
    w_key,
    w_value,
    w_conv_in,
    w_conv_gate,
    sink_logit,
    conv_taps,
    conv_bias,
    channel_gain,
    channel_shift,
    w_attn_out,
    w_conv_out,
):
    rows_here = tokens.shape[0]
    sp_count = lax.axis_size("sp")
    fs_count = lax.axis_size("fs")
    tp_count = lax.axis_size("tp")
    sp_here = lax.axis_index("sp")
    fs_here = lax.axis_index("fs")
    tp_here = lax.axis_index("tp")
    offset = sp_here * rows_here
    total = rows_here * sp_count
    head_tp = w_query.shape[1]
    chan_tp = w_conv_in.shape[1]
    head_cols = head_tp // fs_count
    chan_cols = chan_tp // fs_count
    heads_here = head_cols // HEAD_DIM
    kv_tp = w_key.shape[1] // HEAD_DIM
    group = (head_tp // HEAD_DIM) // kv_tp
    kv_here = max(1, kv_tp // fs_count)
    kv_cols = kv_here * HEAD_DIM
    group_here = heads_here // kv_here
    head_at = fs_here * heads_here
    kv_at = (head_at // group) * HEAD_DIM

    def columns(array, start, size, axis=-1):
        return lax.dynamic_slice_in_dim(array, start, size, axis % array.ndim)

    half = rows_here // tp_count
    token_float = columns(tokens, tp_here * half, half, 0).astype(jnp.float32)
    normed = (
        token_float
        * lax.rsqrt(jnp.mean(token_float * token_float, axis=-1, keepdims=True) + EPSILON)
        * norm_gain[None, :]
    ).astype(jnp.bfloat16)
    packed_in = jnp.concatenate(
        [
            columns(w_query, fs_here * head_cols, head_cols),
            columns(w_conv_in, fs_here * chan_cols, chan_cols),
            columns(w_conv_gate, fs_here * chan_cols, chan_cols),
            columns(w_key, kv_at, kv_cols),
            columns(w_value, kv_at, kv_cols),
        ],
        axis=1,
    )
    packed_out = jnp.concatenate(
        [
            columns(w_attn_out, tp_here * head_tp + fs_here * head_cols, head_cols, 0),
            columns(w_conv_out, tp_here * chan_tp + fs_here * chan_cols, chan_cols, 0),
        ],
        axis=0,
    )
    whole_normed, whole_in = gather_inputs(normed, packed_in)
    whole_out = gather_outputs(packed_out, whole_in)
    acc = jnp.dot(whole_normed, whole_in, preferred_element_type=jnp.float32)
    cut = [head_cols, head_cols + chan_cols, head_cols + 2 * chan_cols]
    cut.append(cut[2] + kv_cols)
    tokens_here = fs_count * rows_here
    positions = offset + jnp.arange(tokens_here, dtype=jnp.int32) % rows_here
    query = grid_rotate(acc[:, : cut[0]].reshape(tokens_here, heads_here, HEAD_DIM), positions)
    keys = grid_rotate(acc[:, cut[2] : cut[3]].reshape(tokens_here, kv_here, HEAD_DIM), positions)
    query = query.astype(jnp.bfloat16)
    keys = keys.astype(jnp.bfloat16).reshape(fs_count, rows_here, kv_cols)
    values = acc[:, cut[3] :].astype(jnp.bfloat16).reshape(fs_count, rows_here, kv_cols)
    glu = (acc[:, cut[0] : cut[1]] * jax.nn.sigmoid(acc[:, cut[1] : cut[2]])).astype(jnp.bfloat16)
    glu = glu.reshape(fs_count, rows_here, chan_cols)
    reach = conv_taps.shape[0] // 2
    rims = padded(glu, (("sp", 1),), reach)
    extended = padded(jnp.concatenate([keys, values], axis=2), (("sp", 1),), WINDOW)
    taps = columns(conv_taps, fs_here * chan_cols, chan_cols)
    bias = columns(conv_bias, fs_here * chan_cols, chan_cols)
    gain = columns(channel_gain, fs_here * chan_cols, chan_cols)
    shift = columns(channel_shift, fs_here * chan_cols, chan_cols)
    filtered = jnp.zeros((fs_count, rows_here, chan_cols), jnp.float32) + bias
    for shift_index in range(conv_taps.shape[0]):
        filtered = filtered + taps[shift_index] * rims[
            :, shift_index : shift_index + rows_here
        ].astype(jnp.float32)
    own_mean = jnp.mean(filtered, axis=-1)
    own_centred = filtered - own_mean[..., None]
    own_square = jnp.sum(own_centred * own_centred, axis=-1)
    pairs = gather_stats(
        jnp.stack([own_mean.reshape(tokens_here), own_square.reshape(tokens_here)])
    )
    centre = jnp.mean(pairs[:, 0], axis=0)
    drift = pairs[:, 0] - centre[None]
    spread = jnp.sum(pairs[:, 1] + chan_cols * (drift * drift), axis=0) / (
        chan_cols * fs_count * tp_count
    )
    centre = centre.reshape(fs_count, rows_here, 1)
    spread = spread.reshape(fs_count, rows_here, 1)

    sinks = columns(sink_logit, head_at, heads_here).reshape(kv_here, group_here)
    sinks = sinks[None, :, :, None, None]
    span = rows_here + 2 * WINDOW
    queries = query.reshape(fs_count, rows_here, kv_here, group_here, HEAD_DIM)
    near_keys = extended[..., :kv_cols].reshape(fs_count, span, kv_here, HEAD_DIM)
    near_values = extended[..., kv_cols:].reshape(fs_count, span, kv_here, HEAD_DIM)
    scores = jnp.einsum(
        "bqkgd,bskd->bkgqs", queries, near_keys, preferred_element_type=jnp.float32
    ) * HEAD_DIM ** (-0.5)
    query_pos = offset + jnp.arange(rows_here, dtype=jnp.int32)
    key_pos = offset - WINDOW + jnp.arange(span, dtype=jnp.int32)
    valid = (
        (jnp.abs(query_pos[:, None] - key_pos[None, :]) <= WINDOW)
        & (key_pos[None, :] >= 0)
        & (key_pos[None, :] < total)
    )
    scores = jnp.where(valid, scores, NEGATIVE)
    top = jnp.maximum(jnp.max(scores, axis=-1, keepdims=True), sinks)
    raised = jnp.exp(scores - top)
    denominator = jnp.sum(raised, axis=-1, keepdims=True) + jnp.exp(sinks - top)
    probs = (raised / denominator).astype(jnp.bfloat16)
    mixed = jnp.einsum("bkgqs,bskd->bqkgd", probs, near_values, preferred_element_type=jnp.float32)
    attended = mixed.astype(jnp.bfloat16).reshape(tokens_here, head_cols)
    conv_out = jax.nn.silu(
        (filtered - centre) * lax.rsqrt(spread + EPSILON) * gain + shift
    ).astype(jnp.bfloat16)
    features = jnp.concatenate([attended, conv_out.reshape(tokens_here, chan_cols)], axis=1)
    return scatter_sum(features, whole_out)


def solution(mesh):
    in_specs = (
        P(("fs", "sp"), None),
        P(),
        P("sp", "tp"),
        P("sp", "tp"),
        P("sp", "tp"),
        P("sp", "tp"),
        P("sp", "tp"),
        P("tp"),
        P(None, "tp"),
        P("tp"),
        P("tp"),
        P("tp"),
        P(None, "sp"),
        P(None, "sp"),
    )
    out_specs = P(("fs", "sp", "tp"), None)
    return jax.shard_map(local, mesh=mesh, in_specs=in_specs, out_specs=out_specs, check_vma=False)
```

```python
import functools

import jax
import jax.numpy as jnp
from jax import lax
from jax.experimental import pallas as pl
from jax.experimental.pallas import tpu as pltpu
from jax.sharding import PartitionSpec as P

MESH = pl.DeviceIdType.MESH
HEAD_DIM = 64
WINDOW = 128
GRID_W = 64


EPSILON = 1e-06
NEGATIVE = -1e30
ROPE_BASE = 10000.0


def padded(block, sides, width):
    for axis, dim in sides:
        count = lax.axis_size(axis)
        forward = [(i, i + 1) for i in range(count - 1)]
        backward = [(target, source) for source, target in forward]
        low = lax.ppermute(
            lax.slice_in_dim(block, block.shape[dim] - width, None, axis=dim), axis, forward
        )
        high = lax.ppermute(lax.slice_in_dim(block, 0, width, axis=dim), axis, backward)
        block = jnp.concatenate([low, block, high], axis=dim)
    return block


def rotate_pairs(values, positions):
    middle = values.shape[-1] // 2
    inverse = ROPE_BASE ** (-jnp.arange(middle, dtype=jnp.float32) / middle)
    angles = positions.astype(jnp.float32)[:, None] * inverse[None, :]
    cosine = jnp.cos(angles)[:, None, :]
    sine_table = jnp.sin(angles)[:, None, :]
    leading = values[..., :middle]
    trailing = values[..., middle:]
    return jnp.concatenate(
        [leading * cosine - trailing * sine_table, leading * sine_table + trailing * cosine],
        axis=-1,
    )


def grid_rotate(values, positions):
    middle = values.shape[-1] // 2
    return jnp.concatenate(
        [
            rotate_pairs(values[..., :middle], positions // GRID_W),
            rotate_pairs(values[..., middle:], positions % GRID_W),
        ],
        axis=-1,
    )


def remote(src, dst, send, recv, **where):
    return pltpu.make_async_remote_copy(
        src_ref=src,
        dst_ref=dst,
        send_sem=send,
        recv_sem=recv,
        device_id=where,
        device_id_type=MESH,
    )


def meet(peers, waits):
    barrier = pltpu.get_barrier_semaphore()
    for condition, where in peers:
        if condition is None:
            pl.semaphore_signal(barrier, inc=1, device_id=where, device_id_type=MESH)
        else:

            @pl.when(condition)
            def _(where=where):
                pl.semaphore_signal(barrier, inc=1, device_id=where, device_id_type=MESH)

    pl.semaphore_wait(barrier, waits)


def input_kernel(
    sizes, own_ref, weight_ref, acc_ref, held, whole, local_sem,
    token_send, token_recv, pass_send, pass_recv, ring_send, ring_recv,
):
    n, fs, tp, chunks = sizes
    me = lax.axis_index("sp")
    f = lax.axis_index("fs")
    t = lax.axis_index("tp")
    depth = weight_ref.shape[0]
    part = depth // chunks
    has_left, has_right = me > 0, me < n - 1
    peers = [(None, {"tp": lax.rem(t + i, tp)}) for i in range(1, tp)]
    peers += [(None, {"fs": lax.rem(f + j, fs)}) for j in range(1, fs)]
    peers += [(has_left, {"sp": me - 1}), (has_right, {"sp": me + 1})]
    meet(peers, tp - 1 + fs - 1 + has_left.astype(jnp.int32) + has_right.astype(jnp.int32))

    def rows(shard, c):
        return pl.ds(pl.multiple_of(shard * depth + c * part, part), part)

    def ring(side, k, c, shard):
        source = (
            weight_ref.at[pl.ds(c * part, part)] if k == 0 else whole.at[rows(shard, c)]
        )
        return remote(
            source, whole.at[rows(shard, c)], ring_send.at[side, k, c],
            ring_recv.at[side, k, c], sp=(me + 1 if side == 0 else me - 1),
        )

    def sends(side, k):
        if side == 0:
            return jnp.logical_and(me - k >= 0, has_right)
        return jnp.logical_and(me + k < n, has_left)

    def shard_sent(side, k):
        return me - k if side == 0 else me + k

    def receives(side, k):
        return me - 1 - k >= 0 if side == 0 else me + 1 + k < n

    def shard_received(side, k):
        return me - 1 - k if side == 0 else me + 1 + k

    for c in range(chunks):
        for side in (0, 1):

            @pl.when(sends(side, 0))
            def _():
                ring(side, 0, c, me).start()

    index = f * tp + t
    token_copies = []
    for j in range(1, fs):
        copy = remote(
            own_ref, held.at[index], token_send.at[j - 1], token_recv.at[j - 1],
            fs=lax.rem(f + j, fs),
        )
        copy.start()
        token_copies.append(copy)
    passes = []
    for i in range(1, tp):
        copy = remote(
            own_ref, held.at[index], pass_send.at[0, i - 1], pass_recv.at[0, i - 1],
            tp=lax.rem(t + i, tp),
        )
        copy.start()
        passes.append(copy)
    stay_token = pltpu.make_async_copy(own_ref, held.at[index], local_sem.at[0])
    stay_token.start()
    stay_weight = pltpu.make_async_copy(
        weight_ref, whole.at[pl.ds(pl.multiple_of(me * depth, depth), depth)], local_sem.at[1]
    )
    stay_weight.start()

    def relay(k):
        for c in range(chunks):
            for side in (0, 1):

                @pl.when(receives(side, k))
                def _():
                    ring(side, k, c, shard_received(side, k)).wait_recv()

                if k + 1 < n - 1:

                    @pl.when(sends(side, k + 1))
                    def _():
                        ring(side, k + 1, c, shard_sent(side, k + 1)).start()

    def tokens_in():
        for j in range(1, fs):
            token_copies[j - 1].wait_recv()
            source = lax.rem(f + fs - j, fs) * tp + t
            for i in range(1, tp):
                copy = remote(
                    held.at[source], held.at[source], pass_send.at[j, i - 1],
                    pass_recv.at[j, i - 1], tp=lax.rem(t + i, tp),
                )
                copy.start()
                passes.append(copy)
        stay_token.wait()
        stay_weight.wait()
        for copy in passes:
            copy.wait_recv()

    blocks, height = held.shape[0], held.shape[1]

    def multiply(column, size, first):
        @pl.loop(0, blocks)
        def _(b):
            place = pl.ds(pl.multiple_of(b * height, height), height)
            term = jnp.dot(
                held[b, :, pl.ds(column, size)],
                whole[pl.ds(column, size), :],
                preferred_element_type=jnp.float32,
            )
            if first:
                acc_ref[place, :] = term
            else:
                acc_ref[place, :] += term

    split = depth % 128 == 0
    early = max(n - 2, 0)
    for k in range(early):
        relay(k)
    tokens_in()
    if split:
        multiply(pl.multiple_of(me * depth, depth), depth, True)
    for k in range(n - 1):
        if k >= early:
            relay(k)
        if split:
            for side in (0, 1):

                @pl.when(receives(side, k))
                def _():
                    shard = shard_received(side, k)
                    multiply(pl.multiple_of(shard * depth, depth), depth, False)

    if not split:
        multiply(0, n * depth, True)
    for copy in token_copies + passes:
        copy.wait_send()
    for k in range(n - 1):
        for c in range(chunks):
            for side in (0, 1):

                @pl.when(sends(side, k))
                def _():
                    ring(side, k, c, shard_sent(side, k)).wait_send()


def gather_project(own, weight):
    n, fs, tp = (lax.axis_size(axis) for axis in ("sp", "fs", "tp"))
    height, width = own.shape
    depth, columns = weight.shape
    chunks = 2 if n <= 8 and depth % 32 == 0 else 1
    steps = max(n - 1, 1)
    dma = pltpu.SemaphoreType.DMA
    return pl.pallas_call(
        functools.partial(input_kernel, (n, fs, tp, chunks)),
        out_shape=jax.ShapeDtypeStruct((fs * tp * height, columns), jnp.float32),
        in_specs=[pl.BlockSpec(memory_space=pltpu.VMEM)] * 2,
        out_specs=pl.BlockSpec(memory_space=pltpu.VMEM),
        scratch_shapes=[
            pltpu.VMEM((fs * tp, height, width), jnp.bfloat16),
            pltpu.VMEM((n * depth, columns), jnp.bfloat16),
            dma((2,)),
            dma((fs - 1,)),
            dma((fs - 1,)),
            dma((fs, tp - 1)),
            dma((fs, tp - 1)),
            dma((2, steps, chunks)),
            dma((2, steps, chunks)),
        ],
        compiler_params=pltpu.CompilerParams(collective_id=0, has_side_effects=True),
    )(own, weight)


def output_kernel(
    sizes, feature_ref, weight_ref, out_ref, part_out, part_in, sum_out, sum_in,
    part_send, part_recv, sum_send, sum_recv,
):
    fs, tp = sizes
    f = lax.axis_index("fs")
    t = lax.axis_index("tp")
    height = out_ref.shape[0]
    peers = [(None, {"tp": lax.rem(t + i, tp)}) for i in range(1, tp)]
    peers += [(None, {"fs": lax.rem(f + j, fs)}) for j in range(1, fs)]
    meet(peers, tp - 1 + fs - 1)

    def term(j, i):
        block = lax.rem(f + j, fs) * tp + lax.rem(t + i, tp)
        place = pl.ds(pl.multiple_of(block * height, height), height)
        return jnp.dot(
            feature_ref[place, :], weight_ref[...], preferred_element_type=jnp.float32
        )

    order = list(range(fs - 1, -1, -1))
    copies = {}
    for j in order:
        for i in range(1, tp):
            part_out[i - 1, j] = term(j, i).astype(jnp.bfloat16)
            copy = remote(
                part_out.at[i - 1, j], part_in.at[i - 1, j], part_send.at[i - 1, j],
                part_recv.at[i - 1, j], tp=lax.rem(t + i, tp),
            )
            copy.start()
            copies[i, j] = copy
    arrivals = []
    for j in order:
        total = term(j, 0)
        for i in range(1, tp):
            copies[i, j].wait_recv()
            total = total + part_in[i - 1, j].astype(jnp.float32)
        if j:
            sum_out[j - 1] = total.astype(jnp.bfloat16)
            copy = remote(
                sum_out.at[j - 1], sum_in.at[j - 1], sum_send.at[j - 1],
                sum_recv.at[j - 1], fs=lax.rem(f + j, fs),
            )
            copy.start()
            arrivals.append((j, copy))
    for j, copy in arrivals:
        copy.wait_recv()
        total = total + sum_in[j - 1].astype(jnp.float32)
    out_ref[...] = total.astype(out_ref.dtype)
    for copy in copies.values():
        copy.wait_send()
    for _, copy in arrivals:
        copy.wait_send()


def scatter_sum(features, whole_out):
    fs, tp = lax.axis_size("fs"), lax.axis_size("tp")
    width = whole_out.shape[1]
    height = features.shape[0] // (fs * tp)
    dma = pltpu.SemaphoreType.DMA
    return pl.pallas_call(
        functools.partial(output_kernel, (fs, tp)),
        out_shape=jax.ShapeDtypeStruct((height, width), jnp.bfloat16),
        in_specs=[pl.BlockSpec(memory_space=pltpu.VMEM)] * 2,
        out_specs=pl.BlockSpec(memory_space=pltpu.VMEM),
        scratch_shapes=[
            pltpu.VMEM((tp - 1, fs, height, width), jnp.bfloat16),
            pltpu.VMEM((tp - 1, fs, height, width), jnp.bfloat16),
            pltpu.VMEM((fs - 1, height, width), jnp.bfloat16),
            pltpu.VMEM((fs - 1, height, width), jnp.bfloat16),
            dma((tp - 1, fs)),
            dma((tp - 1, fs)),
            dma((fs - 1,)),
            dma((fs - 1,)),
        ],
        compiler_params=pltpu.CompilerParams(collective_id=1, has_side_effects=True),
    )(features, whole_out)


def gather_outputs(packed_out):
    n = lax.axis_size("sp")
    if n > 8:
        return lax.all_gather(packed_out, "sp", axis=1, tiled=True)
    me = lax.axis_index("sp")
    pieces = [packed_out]
    for k in range(1, n):
        pieces.append(lax.ppermute(packed_out, "sp", [(i, (i + k) % n) for i in range(n)]))
    pieces = pieces[::-1]
    lined = jnp.concatenate(pieces + pieces[:-1], axis=1)
    width = packed_out.shape[1]
    return lax.dynamic_slice_in_dim(lined, lax.rem(n - 1 - me, n) * width, n * width, 1)


def gather_stats(pair):
    return lax.all_gather(pair, ("fs", "tp"), axis=0)


def local(
    tokens,
    norm_gain,
    w_query,
    w_key,
    w_value,
    w_conv_in,
    w_conv_gate,
    sink_logit,
    conv_taps,
    conv_bias,
    channel_gain,
    channel_shift,
    w_attn_out,
    w_conv_out,
):
    rows_here = tokens.shape[0]
    sp_count = lax.axis_size("sp")
    fs_count = lax.axis_size("fs")
    tp_count = lax.axis_size("tp")
    sp_here = lax.axis_index("sp")
    fs_here = lax.axis_index("fs")
    tp_here = lax.axis_index("tp")
    offset = sp_here * rows_here
    total = rows_here * sp_count
    head_tp = w_query.shape[1]
    chan_tp = w_conv_in.shape[1]
    head_cols = head_tp // fs_count
    chan_cols = chan_tp // fs_count
    heads_here = head_cols // HEAD_DIM
    kv_tp = w_key.shape[1] // HEAD_DIM
    group = (head_tp // HEAD_DIM) // kv_tp
    kv_here = max(1, kv_tp // fs_count)
    kv_cols = kv_here * HEAD_DIM
    group_here = heads_here // kv_here
    head_at = fs_here * heads_here
    kv_at = (head_at // group) * HEAD_DIM

    def columns(array, start, size, axis=-1):
        return lax.dynamic_slice_in_dim(array, start, size, axis % array.ndim)

    half = rows_here // tp_count
    token_float = columns(tokens, tp_here * half, half, 0).astype(jnp.float32)
    normed = (
        token_float
        * lax.rsqrt(jnp.mean(token_float * token_float, axis=-1, keepdims=True) + EPSILON)
        * norm_gain[None, :]
    ).astype(jnp.bfloat16)
    packed_in = jnp.concatenate(
        [
            columns(w_query, fs_here * head_cols, head_cols),
            columns(w_conv_in, fs_here * chan_cols, chan_cols),
            columns(w_conv_gate, fs_here * chan_cols, chan_cols),
            columns(w_key, kv_at, kv_cols),
            columns(w_value, kv_at, kv_cols),
        ],
        axis=1,
    )
    packed_out = jnp.concatenate(
        [
            columns(w_attn_out, tp_here * head_tp + fs_here * head_cols, head_cols, 0),
            columns(w_conv_out, tp_here * chan_tp + fs_here * chan_cols, chan_cols, 0),
        ],
        axis=0,
    )
    acc = gather_project(normed, packed_in)
    acc, packed_out = lax.optimization_barrier((acc, packed_out))
    whole_out = gather_outputs(packed_out)
    cut = [head_cols, head_cols + chan_cols, head_cols + 2 * chan_cols]
    cut.append(cut[2] + kv_cols)
    tokens_here = fs_count * rows_here
    positions = offset + jnp.arange(tokens_here, dtype=jnp.int32) % rows_here
    query = grid_rotate(acc[:, : cut[0]].reshape(tokens_here, heads_here, HEAD_DIM), positions)
    keys = grid_rotate(acc[:, cut[2] : cut[3]].reshape(tokens_here, kv_here, HEAD_DIM), positions)
    query = query.astype(jnp.bfloat16)
    keys = keys.astype(jnp.bfloat16).reshape(fs_count, rows_here, kv_cols)
    values = acc[:, cut[3] :].astype(jnp.bfloat16).reshape(fs_count, rows_here, kv_cols)
    glu = (acc[:, cut[0] : cut[1]] * jax.nn.sigmoid(acc[:, cut[1] : cut[2]])).astype(jnp.bfloat16)
    glu = glu.reshape(fs_count, rows_here, chan_cols)
    reach = conv_taps.shape[0] // 2
    rims = padded(glu, (("sp", 1),), reach)
    extended = padded(jnp.concatenate([keys, values], axis=2), (("sp", 1),), WINDOW)
    taps = columns(conv_taps, fs_here * chan_cols, chan_cols)
    bias = columns(conv_bias, fs_here * chan_cols, chan_cols)
    gain = columns(channel_gain, fs_here * chan_cols, chan_cols)
    shift = columns(channel_shift, fs_here * chan_cols, chan_cols)
    filtered = jnp.zeros((fs_count, rows_here, chan_cols), jnp.float32) + bias
    for shift_index in range(conv_taps.shape[0]):
        filtered = filtered + taps[shift_index] * rims[
            :, shift_index : shift_index + rows_here
        ].astype(jnp.float32)
    own_mean = jnp.mean(filtered, axis=-1)
    own_centred = filtered - own_mean[..., None]
    own_square = jnp.sum(own_centred * own_centred, axis=-1)
    pairs = gather_stats(
        jnp.stack([own_mean.reshape(tokens_here), own_square.reshape(tokens_here)])
    )
    centre = jnp.mean(pairs[:, 0], axis=0)
    drift = pairs[:, 0] - centre[None]
    spread = jnp.sum(pairs[:, 1] + chan_cols * (drift * drift), axis=0) / (
        chan_cols * fs_count * tp_count
    )
    centre = centre.reshape(fs_count, rows_here, 1)
    spread = spread.reshape(fs_count, rows_here, 1)

    sinks = columns(sink_logit, head_at, heads_here).reshape(kv_here, group_here)
    sinks = sinks[None, :, :, None, None]
    span = rows_here + 2 * WINDOW
    queries = query.reshape(fs_count, rows_here, kv_here, group_here, HEAD_DIM)
    near_keys = extended[..., :kv_cols].reshape(fs_count, span, kv_here, HEAD_DIM)
    near_values = extended[..., kv_cols:].reshape(fs_count, span, kv_here, HEAD_DIM)
    scores = jnp.einsum(
        "bqkgd,bskd->bkgqs", queries, near_keys, preferred_element_type=jnp.float32
    ) * HEAD_DIM ** (-0.5)
    query_pos = offset + jnp.arange(rows_here, dtype=jnp.int32)
    key_pos = offset - WINDOW + jnp.arange(span, dtype=jnp.int32)
    valid = (
        (jnp.abs(query_pos[:, None] - key_pos[None, :]) <= WINDOW)
        & (key_pos[None, :] >= 0)
        & (key_pos[None, :] < total)
    )
    scores = jnp.where(valid, scores, NEGATIVE)
    top = jnp.maximum(jnp.max(scores, axis=-1, keepdims=True), sinks)
    raised = jnp.exp(scores - top)
    denominator = jnp.sum(raised, axis=-1, keepdims=True) + jnp.exp(sinks - top)
    probs = (raised / denominator).astype(jnp.bfloat16)
    mixed = jnp.einsum("bkgqs,bskd->bqkgd", probs, near_values, preferred_element_type=jnp.float32)
    attended = mixed.astype(jnp.bfloat16).reshape(tokens_here, head_cols)
    conv_out = jax.nn.silu(
        (filtered - centre) * lax.rsqrt(spread + EPSILON) * gain + shift
    ).astype(jnp.bfloat16)
    features = jnp.concatenate([attended, conv_out.reshape(tokens_here, chan_cols)], axis=1)
    return scatter_sum(features, whole_out)


def solution(mesh):
    in_specs = (
        P(("fs", "sp"), None),
        P(),
        P("sp", "tp"),
        P("sp", "tp"),
        P("sp", "tp"),
        P("sp", "tp"),
        P("sp", "tp"),
        P("tp"),
        P(None, "tp"),
        P("tp"),
        P("tp"),
        P("tp"),
        P(None, "sp"),
        P(None, "sp"),
    )
    out_specs = P(("fs", "sp", "tp"), None)
    return jax.shard_map(local, mesh=mesh, in_specs=in_specs, out_specs=out_specs, check_vma=False)
```
